32 devices in a mesh: rep: 2 (over x), fs: 8 (over z, y), tp: 2 (over core).
Axes of the slice: x: 2, y: 2, z: 4, core: 2. Of those that a mesh axis runs over, the one named last changes fastest.
Arguments:
- tokens: bfloat16 [5120, 2048], P(('rep', 'fs')), may hold values from -6 to 6
- mixer_out: bfloat16 [5120, 2048], P(('rep', 'fs')), may hold values from -6 to 6
- gate_first: bfloat16 [2048, 2816], P('fs', 'tp'), may hold values from -0.125 to 0.125
- up_first: bfloat16 [2048, 2816], P('fs', 'tp'), may hold values from -0.125 to 0.125
- down_first: bfloat16 [2816, 2048], P('tp', 'fs'), may hold values from -0.3125 to 0.3125
- gate_second: bfloat16 [2048, 2816], P('fs', 'tp'), may hold values from -0.125 to 0.125
- up_second: bfloat16 [2048, 2816], P('fs', 'tp'), may hold values from -0.125 to 0.125
- down_second: bfloat16 [2816, 2048], P('tp', 'fs'), may hold values from -0.3125 to 0.3125
- gain_first: float32 [2048], replicated, may hold values from 0.1 to 1.9
- bias_first: float32 [2048], replicated, may hold values from -1.5 to 1.5
- gain_middle: float32 [2048], replicated, may hold values from 0.1 to 1.9
- bias_middle: float32 [2048], replicated, may hold values from -1.5 to 1.5
- gain_last: float32 [2048], replicated, may hold values from 0.1 to 1.9
- bias_last: float32 [2048], replicated, may hold values from -1.5 to 1.5
Outputs:
- layer_out: bfloat16 [5120, 2048], P(('rep', 'fs'))
The draws below stay inside these ranges and needn't reach their ends.
All inputs are finite; a program needn't handle non-finite values.
Results may differ from the reference program's by a relative error of at most 0.014.
Values may be sent and summed in bfloat16 or wider, within the bound.
No kernel may reach another device: no remote copies, remote signals or barrier semaphores. Data moves between devices by JAX's collectives and lax.ppermute only.
A program may use at most 64 MiB of HBM per device.

```python
import math
import jax
import jax.numpy as jnp
from jax import lax

D = 2048
FF = 2816
TOKENS = 5120
N_TP = 2


def level_of(own_key, extent, shards, low, high):
    loudness, own = 1.0, jax.random.fold_in(own_key, 6)
    for axis_at, parts in shards:
        draws = jnp.exp(jax.random.uniform(jax.random.fold_in(own, axis_at), (parts,), jnp.float32, low / len(shards), high / len(shards)))
        loudness = loudness * jnp.repeat(draws, extent[axis_at] // parts).reshape([-1 if axis == axis_at else 1 for axis in range(len(extent))])
    return loudness


def normal_values(own_key, shape, width, bound, cuts=(), kind=jnp.bfloat16):
    result = width * jax.random.normal(own_key, shape, jnp.float32)
    if cuts:
        result = result * level_of(own_key, shape, cuts, -0.22, 0.18)
    return jnp.clip(result, -bound, bound).astype(kind)


def setup_inputs(seed: int = 0) -> dict:
    seeds = jax.random.split(jax.random.key(seed), 15)
    tokens = normal_values(seeds[0], (TOKENS, D), 1.0, 6.0, ((0, 16),))
    mixer_out = normal_values(seeds[1], (TOKENS, D), 1.0, 6.0, ((0, 16),))
    gate_first = normal_values(seeds[2], (D, FF), D ** -0.5, 0.125, ((0, 8), (1, 2)))
    up_first = normal_values(seeds[3], (D, FF), D ** -0.5, 0.125, ((0, 8), (1, 2)))
    down_first = normal_values(seeds[4], (FF, D), (FF // 8) ** -0.5, 0.3125, ((0, 2), (1, 8)))
    gate_second = normal_values(seeds[5], (D, FF), D ** -0.5, 0.125, ((0, 8), (1, 2)))
    up_second = normal_values(seeds[6], (D, FF), D ** -0.5, 0.125, ((0, 8), (1, 2)))
    down_second = normal_values(seeds[7], (FF, D), (FF // 8) ** -0.5, 0.3125, ((0, 2), (1, 8)))
    gain_first = jnp.clip(1.0 + 0.18 * jax.random.normal(seeds[8], (D,), jnp.float32), 0.1, 1.9)
    bias_first = normal_values(seeds[9], (D,), 0.3, 1.5, (), jnp.float32)
    gain_middle = jnp.clip(1.0 + 0.18 * jax.random.normal(seeds[10], (D,), jnp.float32), 0.1, 1.9)
    bias_middle = normal_values(seeds[11], (D,), 0.3, 1.5, (), jnp.float32)
    gain_last = jnp.clip(1.0 + 0.18 * jax.random.normal(seeds[12], (D,), jnp.float32), 0.1, 1.9)
    bias_last = normal_values(seeds[13], (D,), 0.3, 1.5, (), jnp.float32)
    return dict(tokens=tokens, mixer_out=mixer_out, gate_first=gate_first, up_first=up_first, down_first=down_first, gate_second=gate_second, up_second=up_second, down_second=down_second, gain_first=gain_first, bias_first=bias_first, gain_middle=gain_middle, bias_middle=bias_middle, gain_last=gain_last, bias_last=bias_last)


residual_scale = math.sqrt(2.0)
norm_eps = 1e-05

def normalize(summed, scaling, offset):
    center = summed - lax.optimization_barrier(jnp.mean(summed, axis=-1, keepdims=True))
    spread = lax.optimization_barrier(jnp.mean(center * center, axis=-1, keepdims=True))
    return center * lax.rsqrt(spread + norm_eps) * scaling.astype(jnp.float32) + offset.astype(jnp.float32)

def half_step(inputs, gate_weight, up_weight, down_weight):
    gate = jnp.dot(inputs, gate_weight, preferred_element_type=jnp.float32)
    value = jnp.dot(inputs, up_weight, preferred_element_type=jnp.float32)
    hidden = (jax.nn.silu(gate) * value).astype(jnp.bfloat16)
    block_size = hidden.shape[1] // N_TP
    running = jnp.zeros((inputs.shape[0], down_weight.shape[1]), jnp.float32)
    for member in range(N_TP):
        partial_value = jnp.dot(hidden[:, member * block_size:(member + 1) * block_size], down_weight[member * block_size:(member + 1) * block_size], preferred_element_type=jnp.float32)
        running = running + partial_value.astype(jnp.bfloat16).astype(jnp.float32)
    return running.astype(jnp.bfloat16)

def reference(tokens, mixer_out, gate_first, up_first, down_first, gate_second, up_second, down_second, gain_first, bias_first, gain_middle, bias_middle, gain_last, bias_last):
    first_branch = half_step(tokens, gate_first, up_first, down_first)
    first_norm = normalize(residual_scale * tokens.astype(jnp.float32) + 0.5 * first_branch.astype(jnp.float32), gain_first, bias_first).astype(jnp.bfloat16)
    middle_norm = normalize(residual_scale * first_norm.astype(jnp.float32) + mixer_out.astype(jnp.float32), gain_middle, bias_middle).astype(jnp.bfloat16)
    second_branch = half_step(middle_norm, gate_second, up_second, down_second)
    return normalize(residual_scale * middle_norm.astype(jnp.float32) + 0.5 * second_branch.astype(jnp.float32), gain_last, bias_last).astype(jnp.bfloat16)
```

```python
import math

import jax
import jax.numpy as jnp
from jax import lax
from jax.sharding import PartitionSpec as P

residual_scale = math.sqrt(2.0)
norm_eps = 1e-05
bf16, f32 = jnp.bfloat16, jnp.float32


def make_body(R, F, C):
    m = F // 2
    NG = 2 * R

    def body(tokens, mixer_out, gate_first, up_first, down_first, gate_second,
             up_second, down_second, gain_first, bias_first, gain_middle,
             bias_middle, gain_last, bias_last):
        a = lax.axis_index("rep")
        i = lax.axis_index("fs")
        c = lax.axis_index("tp")
        z, b = i // 2, i % 2
        g = a * 2 + b

        def pair_swap(x):
            return lax.ppermute(x, "fs", [(j, j ^ 1) for j in range(F)])

        def tp_shift(x, k):
            return lax.ppermute(x, "tp", [(j, (j + k) % C) for j in range(C)])

        def plane_xor(x, k, only=None):
            pairs = [(j, j ^ (2 * k)) for j in range(F) if only is None or (j // 2) in only]
            return lax.ppermute(x, "fs", pairs)

        def group_xor(x, d):
            dr, dy = d // 2, d % 2
            pairs = [(r * F + j, (r ^ dr) * F + (j ^ dy)) for r in range(R) for j in range(F)]
            return lax.ppermute(x, ("rep", "fs"), pairs)

        rows = tokens.shape[0]
        h = rows // C
        D = tokens.shape[1]
        kb = D // m
        ffl = gate_first.shape[1]
        piece = ffl // NG

        hid = lax.broadcasted_iota(jnp.int32, (piece, ffl), 1)
        row = lax.broadcasted_iota(jnp.int32, (piece, ffl), 0)

        def pick_in(w, which):
            sel = (hid == row + which * piece).astype(bf16)
            return lax.dot_general(sel, w, (((1,), (1,)), ((), ())),
                                   preferred_element_type=f32).astype(bf16)

        def pick_down(w, which):
            return lax.dynamic_slice_in_dim(w, which * piece, piece, axis=0)

        def ordered(own, other):
            lo = jnp.where(b == 0, own, other)
            hi = jnp.where(b == 0, other, own)
            return jnp.concatenate([lo, hi], axis=1)

        mine, theirs = g, a * 2 + (1 - b)

        def in_block(gw, uw):
            own = jnp.concatenate([pick_in(gw, mine), pick_in(uw, mine)], axis=0)
            away = jnp.concatenate([pick_in(gw, theirs), pick_in(uw, theirs)], axis=0)
            return ordered(own, pair_swap(away))

        def down_block(dw):
            return ordered(pick_down(dw, mine), pair_swap(pick_down(dw, theirs)))

        def planes(x):
            if m != 4:
                return [x] + [plane_xor(x, k) for k in range(1, m)]
            one = plane_xor(x, 1)
            two = plane_xor(x, 2)
            mid = plane_xor(x, 3, only=(1, 2))
            far = lax.ppermute(two, "fs", [(2, 0), (3, 1), (4, 6), (5, 7)])
            three = jnp.where((z == 1) | (z == 2), mid, far)
            return [x, one, two, three]

        def half(x):
            return lax.dynamic_slice_in_dim(x, c * h, h, axis=0)

        def by_block(x):
            return x.reshape(x.shape[0], m, kb).transpose(1, 0, 2)

        def gather_tokens(x):
            same = jnp.concatenate([x] + [group_xor(x, d) for d in range(1, NG)], axis=1)
            return jnp.concatenate([same] + [tp_shift(same, k) for k in range(1, C)], axis=1)

        def block_of(x, k):
            return lax.dynamic_index_in_dim(x, z ^ k, 0, keepdims=False)

        def contract(x, w):
            return lax.dot_general(x, w, (((1,), (1,)), ((), ())), preferred_element_type=f32)

        def hidden_of(u, ws):
            gate = up = None
            for k in range(m):
                x = block_of(u, k)
                p, q = contract(x, ws[k][:piece]), contract(x, ws[k][piece:])
                gate = p if gate is None else gate + p
                up = q if up is None else up + q
            return (jax.nn.silu(gate) * up).astype(bf16)

        def scatter_sum(part):
            part = part.astype(bf16)
            n = NG * h
            acc = part[:n].astype(f32)
            for k in range(1, C):
                acc = acc + tp_shift(part[(C - k) * n:(C - k + 1) * n], k).astype(f32)
            acc16 = acc.astype(bf16)
            out = acc[:h]
            for d in range(1, NG):
                out = out + group_xor(acc16[d * h:(d + 1) * h], d).astype(f32)
            return out

        def feed_forward(u, wi, wd):
            hid16 = hidden_of(u, wi)
            outs = []
            for k in range(m):
                part = jnp.dot(hid16, wd[k], preferred_element_type=f32)
                outs.append(scatter_sum(part).astype(bf16))
            return outs

        def natural(outs):
            st = jnp.stack(outs)
            return jnp.stack([lax.dynamic_index_in_dim(st, z ^ j, 0, keepdims=False)
                              for j in range(m)])

        def vec(v):
            return v.reshape(m, 1, kb)

        def norm(x, gain, bias):
            center = x - jnp.mean(x, axis=(0, 2), keepdims=True)
            spread = jnp.mean(center * center, axis=(0, 2), keepdims=True)
            return center * lax.rsqrt(spread + norm_eps) * vec(gain) + vec(bias)

        tok = by_block(half(tokens))
        mix = by_block(half(mixer_out))
        w1 = planes(in_block(gate_first, up_first))
        u1 = gather_tokens(tok)
        d1 = planes(down_block(down_first))
        w2 = planes(in_block(gate_second, up_second))
        d2 = planes(down_block(down_second))

        branch = natural(feed_forward(u1, w1, d1)).astype(f32)
        first_norm = norm(residual_scale * tok.astype(f32) + 0.5 * branch,
                          gain_first, bias_first).astype(bf16)
        middle = norm(residual_scale * first_norm.astype(f32) + mix.astype(f32),
                      gain_middle, bias_middle).astype(bf16)
        u2 = gather_tokens(middle)
        branch = natural(feed_forward(u2, w2, d2)).astype(f32)
        done = norm(residual_scale * middle.astype(f32) + 0.5 * branch,
                    gain_last, bias_last).astype(bf16)
        done = done.transpose(1, 0, 2).reshape(h, D)
        st = jnp.stack([done] + [tp_shift(done, k) for k in range(1, C)])
        return jnp.concatenate([lax.dynamic_index_in_dim(st, (c - j) % C, 0, keepdims=False)
                                for j in range(C)], axis=0)

    return body


def solution(mesh):
    R, F, C = mesh.shape["rep"], mesh.shape["fs"], mesh.shape["tp"]
    tok = P(("rep", "fs"), None)
    win, wout = P("fs", "tp"), P("tp", "fs")
    return jax.shard_map(
        make_body(R, F, C),
        mesh=mesh,
        in_specs=(tok, tok, win, win, wout, win, win, wout) + (P(),) * 6,
        out_specs=tok,
        check_vma=False,
    )
```

```python
import functools
import math

import jax
import jax.numpy as jnp
from jax import lax
from jax.experimental import pallas as pl
from jax.experimental.pallas import tpu as pltpu
from jax.sharding import PartitionSpec as P


residual_scale = math.sqrt(2.0)
norm_eps = 1e-05
bf16, f32 = jnp.bfloat16, jnp.float32


def normalize(summed, scaling, offset):
    center = summed - jnp.mean(summed, axis=-1, keepdims=True)
    spread = jnp.mean(center * center, axis=-1, keepdims=True)
    return center * lax.rsqrt(spread + norm_eps) * scaling + offset


def half_step(inputs, gate_weight, up_weight, down_weight):
    gate = jnp.dot(inputs, lax.all_gather(gate_weight, "fs", axis=0, tiled=True),
                   preferred_element_type=f32)
    value = jnp.dot(inputs, lax.all_gather(up_weight, "fs", axis=0, tiled=True),
                    preferred_element_type=f32)
    hidden = (jax.nn.silu(gate) * value).astype(bf16)
    partials = jnp.dot(hidden, lax.all_gather(down_weight, "fs", axis=1, tiled=True),
                       preferred_element_type=f32)
    return lax.psum(partials.astype(bf16), "tp")


def plain(tokens, mixer_out, gate_first, up_first, down_first, gate_second, up_second,
          down_second, gain_first, bias_first, gain_middle, bias_middle, gain_last, bias_last):
    branch = half_step(tokens, gate_first, up_first, down_first).astype(f32)
    first_norm = normalize(residual_scale * tokens.astype(f32) + 0.5 * branch,
                           gain_first, bias_first).astype(bf16)
    middle = normalize(residual_scale * first_norm.astype(f32) + mixer_out.astype(f32),
                       gain_middle, bias_middle).astype(bf16)
    branch = half_step(middle, gate_second, up_second, down_second).astype(f32)
    return normalize(residual_scale * middle.astype(f32) + 0.5 * branch,
                     gain_last, bias_last).astype(bf16)


PLANES, CHIPS = 4, 4


def place():
    i = lax.axis_index("fs")
    return i // 2, i % 2


def nt(x, w):
    return lax.dot_general(x, w, (((1,), (1,)), ((), ())), preferred_element_type=f32)


def pick_in_kernel(gate_ref, up_ref, *outs):
    piece = outs[0].shape[0] // 2
    _, b = place()
    a = lax.axis_index("rep")
    width = min(gate_ref.shape[1], (piece + 254) // 128 * 128)
    row = lax.broadcasted_iota(jnp.int32, (piece, width), 0)
    col = lax.broadcasted_iota(jnp.int32, (piece, width), 1)
    for out, kind in zip(outs, (0, 1)):
        which = 2 * a + (b ^ kind)
        at = jnp.minimum(which * piece // 128 * 128, gate_ref.shape[1] - width)
        at = pl.multiple_of(at, 128)
        pick = jnp.where(col == row + (which * piece - at), 1.0, 0.0).astype(bf16)
        out[:piece] = nt(pick, gate_ref[:, pl.ds(at, width)]).astype(bf16)
        out[piece:] = nt(pick, up_ref[:, pl.ds(at, width)]).astype(bf16)


def pick_down_kernel(down_ref, own_ref, away_ref):
    piece = own_ref.shape[0]
    _, b = place()
    a = lax.axis_index("rep")
    own_ref[...] = down_ref[pl.ds((2 * a + b) * piece, piece), :]
    away_ref[...] = down_ref[pl.ds((2 * a + 1 - b) * piece, piece), :]


def vm(shape, dtype):
    return jax.ShapeDtypeStruct(shape, dtype)


def pick_in(gate, up):
    kb, ffl = gate.shape
    piece = ffl // CHIPS
    return pl.pallas_call(
        pick_in_kernel, out_shape=(vm((2 * piece, kb), bf16),) * 2, name="pick_in")(gate, up)


def pick_down(down):
    ffl, kb = down.shape
    piece = ffl // CHIPS
    return pl.pallas_call(
        pick_down_kernel, out_shape=(vm((piece, kb), bf16),) * 2, name="pick_down")(down)


def start_all(copies):
    for cp in copies:
        cp.start()
    return copies


def finish(copies):
    for cp in copies:
        cp.wait()


def hidden_kernel(n_tok, split, n_down, *refs):
    toks, refs = refs[:n_tok], refs[n_tok:]
    nw = 10 if split else 5
    ws, refs = refs[:nw], refs[nw:]
    downs, refs = refs[:n_down], refs[n_down:]
    outs, refs = refs[:2], refs[2:]
    lined, refs = (refs[0], refs[1:]) if n_down else (None, refs)
    u, w, sem = refs
    h = toks[0].shape[0]
    kb = w.shape[1] // (2 * PLANES)
    piece = w.shape[0] // 2
    z, b = place()
    tok_copies = [pltpu.make_async_copy(t, u.at[pl.ds(n * h, h)], sem.at[n])
                  for n, t in enumerate(toks)]

    def put(ref, k, s, n):
        at = pl.multiple_of((2 * (z ^ k) + (b ^ s)) * kb, kb)
        return pltpu.make_async_copy(ref, w.at[:, pl.ds(at, kb)], sem.at[n])

    def part(n, s):
        return ws[2 * n + s] if split else ws[n].at[s]

    last = n_tok + 6
    start_all(tok_copies[:2])
    copies = start_all([put(part(k, s), k, s, n_tok + 2 * k + s)
                        for k in range(3) for s in range(2)])
    middle = (z == 1) | (z == 2)
    for cond, src in ((middle, 3), (jnp.logical_not(middle), 4)):
        @pl.when(cond)
        def _():
            start_all([put(part(src, s), 3, s, last + s) for s in range(2)])
    start_all(tok_copies[2:])
    lining = start_all([
        pltpu.make_async_copy(ref, lined.at[:, n * ref.shape[1]:(n + 1) * ref.shape[1]],
                              sem.at[last + 2 + n]) for n, ref in enumerate(downs)])
    finish(copies)
    finish([put(part(3, s), 3, s, last + s) for s in range(2)])
    each = n_tok // 2
    for n in range(0, n_tok, 2):
        finish(tok_copies[n:n + 2])
        x = u[n * h:(n + 2) * h]
        gate = nt(x, w[:piece])
        up = nt(x, w[piece:])
        hid = (gate / (1.0 + jnp.exp(-gate)) * up).astype(bf16)
        for i in range(2):
            to, at = divmod(n + i, each)
            outs[to][at * h:(at + 1) * h] = hid[i * h:(i + 1) * h]
    finish(lining)


def hidden(own_toks, other_toks, ws, downs=()):
    toks = list(own_toks) + list(other_toks)
    split = len(ws) == 10
    h, D = toks[0].shape
    rows2 = ws[0].shape[-2]
    M = len(toks) * h
    hbm, vmem = pl.BlockSpec(memory_space=pltpu.HBM), pl.BlockSpec(memory_space=pltpu.VMEM)
    lined = [vm((rows2 // 2, D), bf16)] if downs else []
    return pl.pallas_call(
        functools.partial(hidden_kernel, len(toks), split, len(downs)),
        in_specs=[hbm] * (len(toks) + len(ws) + len(downs)),
        out_specs=[vmem, vmem] + [vmem] * len(lined),
        out_shape=[vm((M // 2, rows2 // 2), bf16)] * 2 + lined,
        scratch_shapes=[pltpu.VMEM((M, D), bf16), pltpu.VMEM((rows2, D), bf16),
                        pltpu.SemaphoreType.DMA((len(toks) + 8 + len(downs),))])(*toks, *ws, *downs)


def norm(parts, gain_ref, bias_ref):
    width = sum(p.shape[1] for p in parts)
    mean = sum(jnp.sum(p, axis=1, keepdims=True) for p in parts) / width
    parts = [p - mean for p in parts]
    var = sum(jnp.sum(p * p, axis=1, keepdims=True) for p in parts) / width
    inv = lax.rsqrt(var + norm_eps)
    at, out = 0, []
    for p in parts:
        n = p.shape[1]
        out.append(p * inv * gain_ref[:, at:at + n] + bias_ref[:, at:at + n])
        at += n
    return out


def norm_kernel(two, step, own, y, x, d, res_ref, *refs):
    if two:
        mix_ref, refs = refs[0], refs[1:]
    *vectors, out_ref, s = refs
    z, b = place()
    nb, h, kb = s.shape
    for i in range(PLANES):
        for t in range(2):
            at, flip = (2 * i + t) * kb, (2 * i + 1 - t) * kb
            s[2 * (z ^ i) + (b ^ t)] = (
                (own[:, at:at + kb] + x[:, at:at + kb].astype(f32))
                + (y[:, flip:flip + kb].astype(f32) + d[:, flip:flip + kb].astype(f32)))

    def body(r, _):
        rows = pl.ds(pl.multiple_of(r * step, step), step)
        parts = [residual_scale * res_ref[rows, j * kb:(j + 1) * kb].astype(f32)
                 + 0.5 * s[j, rows].astype(bf16).astype(f32) for j in range(nb)]
        parts = norm(parts, vectors[0], vectors[1])
        if two:
            parts = [residual_scale * p.astype(bf16).astype(f32)
                     + mix_ref[rows, j * kb:(j + 1) * kb].astype(f32)
                     for j, p in enumerate(parts)]
            parts = norm(parts, vectors[2], vectors[3])
        for j, p in enumerate(parts):
            out_ref[rows, j * kb:(j + 1) * kb] = p.astype(bf16)
        return 0

    lax.fori_loop(0, h // step, body, 0, unroll=True)


def norm_call(sums, arrays, vectors):
    h, D = arrays[0].shape
    vectors = [v.reshape(1, D) for v in vectors]
    return pl.pallas_call(
        functools.partial(norm_kernel, len(arrays) == 2, 32), out_shape=vm((h, D), bf16),
        scratch_shapes=[pltpu.VMEM((2 * PLANES, h, D // (2 * PLANES)), f32)])(*sums, *arrays, *vectors)


def grouped(R, F, C):
    def named(x, axes, pairs):
        return lax.ppermute(x, axes, pairs)

    def pair_swap(x):
        return named(x, "fs", [(j, j ^ 1) for j in range(F)])

    def group_xor(x, d):
        return named(x, ("rep", "fs"),
                     [(r * F + j, (r ^ (d // 2)) * F + (j ^ (d % 2)))
                      for r in range(R) for j in range(F)])

    def tp_swap(x):
        return named(x, "tp", [(j, j ^ 1) for j in range(C)])

    def plane_xor(x, k, only=None):
        return named(x, "fs",
                     [(j, j ^ (2 * k)) for j in range(F) if only is None or (j // 2) in only])

    def planes(x):
        two = plane_xor(x, 2)
        one = plane_xor(x, 1)
        mid = plane_xor(x, 3, only=(1, 2))
        far = named(two, "fs", [(2, 0), (3, 1), (4, 6), (5, 7)])
        return [x, one, two, mid, far]

    def share(x):
        got = [x] + [group_xor(x, d) for d in (1, 2, 3)]
        return got, [tp_swap(v) for v in got]

    def down_away(q, w):
        part = jnp.dot(q, w, preferred_element_type=f32).astype(bf16)
        return tp_swap(part)

    def down_own(mine, w, got):
        return got.astype(f32) + jnp.dot(mine, w, preferred_element_type=f32)

    def feed(own, other, w_in, w_down):
        h = own[0].shape[0]
        z, _ = place()
        d_own, one, two, mid, far = w_down
        mine_n, theirs_n, w = hidden(own[1:3], other[1:3], w_in, (d_own, one, two))
        three = jnp.where((z == 1) | (z == 2), mid, far)
        w = lax.dynamic_update_slice(w, three, (0, 3 * three.shape[1]))
        mine_o, theirs_o = hidden(own[:1], other[:1], w_in)
        mine_d, theirs_d = hidden(own[3:], other[3:], w_in)
        sums = []
        for mine, theirs, at in ((mine_o, theirs_o, 0), (mine_n, theirs_n, 0),
                                                (mine_n, theirs_n, h), (mine_d, theirs_d, 0)):
            got = down_away(theirs[at:at + h], w)
            sums.append(down_own(mine[at:at + h], w, got))
        return [sums[0]] + [group_xor(sums[d].astype(bf16), d) for d in (1, 2, 3)]

    def body(tokens, mixer_out, gate_first, up_first, down_first, gate_second, up_second,
             down_second, gain_first, bias_first, gain_middle, bias_middle, gain_last, bias_last):
        c = lax.axis_index("tp")
        h = tokens.shape[0] // C
        tok = lax.dynamic_slice_in_dim(tokens, c * h, h, axis=0)
        mix = lax.dynamic_slice_in_dim(mixer_out, c * h, h, axis=0)

        own, away = pick_in(gate_first, up_first)
        got = pair_swap(away)
        g1o = planes(own)
        d_own, d_away = pick_down(down_first)
        d_got = pair_swap(d_away)
        own_t, other_t = share(tok)
        g1r = planes(got)
        d1 = planes(jnp.concatenate([d_own, d_got], axis=1))
        g2_own, g2_away = pick_in(gate_second, up_second)
        g2_got = pair_swap(g2_away)
        d2_own, d2_away = pick_down(down_second)
        d2_got = pair_swap(d2_away)
        g2 = jnp.stack([g2_own, g2_got])
        d2 = jnp.concatenate([d2_own, d2_got], axis=1)
        g2, d2 = planes(g2), planes(d2)
        g1 = [v for pair in zip(g1o, g1r) for v in pair]

        sums = feed(own_t, other_t, g1, d1)
        middle = norm_call(sums, (tok, mix), (gain_first, bias_first, gain_middle, bias_middle))
        own_t, other_t = share(middle)
        sums = feed(own_t, other_t, g2, d2)
        done = norm_call(sums, (middle,), (gain_last, bias_last))
        whole = lax.dynamic_update_slice_in_dim(jnp.zeros_like(tokens), done, c * h, axis=0)
        return lax.dynamic_update_slice_in_dim(whole, tp_swap(done), (1 - c) * h, axis=0)

    return body


def solution(mesh):
    R, F, C = mesh.shape["rep"], mesh.shape["fs"], mesh.shape["tp"]
    tok = P(("rep", "fs"), None)
    win, wout = P("fs", "tp"), P("tp", "fs")
    fast = (R, F, C) == (2, 2 * PLANES, 2)
    return jax.shard_map(
        grouped(R, F, C) if fast else plain,
        mesh=mesh,
        in_specs=(tok, tok, win, win, wout, win, win, wout) + (P(),) * 6,
        out_specs=tok,
        check_vma=False,
    )
```
